32 devices in a mesh: sp: 8 (over z, x), tp: 4 (over y, core).
Axes of the slice: x: 2, y: 2, z: 4, core: 2. Of those that a mesh axis runs over, the one named last changes fastest.
Arguments:
- resid: bfloat16 [2048, 4096], P('sp'), may hold values from -6 to 6
- queries: bfloat16 [2048, 3072], P('sp', 'tp'), may hold values from -1000 to 1000
- latent: bfloat16 [2048, 512], P('sp'), may hold values from -6 to 6
- rope_key: bfloat16 [2048, 64], P('sp'), may hold values from -6 to 6
- lat_gain: float32 [512], replicated, may hold values from 0.1 to 1.9
- kv_weight: bfloat16 [512, 4096], P(None, 'tp'), may hold values from -4 to 4
- out_gain: float32 [2048], P('tp'), may hold values from 0.1 to 1.9
- out_weight: bfloat16 [2048, 4096], P('tp'), may hold values from -0.125 to 0.125
- ffn_gain: float32 [4096], replicated, may hold values from 0.1 to 1.9
- gate_weight: bfloat16 [4096, 6144], P('sp', 'tp'), may hold values from -0.09375 to 0.09375
- up_weight: bfloat16 [4096, 6144], P('sp', 'tp'), may hold values from -0.09375 to 0.09375
- down_weight: bfloat16 [6144, 4096], P('tp', 'sp'), may hold values from -0.078125 to 0.078125
Outputs:
- result: bfloat16 [2048, 4096], P(('sp', 'tp'))
The draws below stay inside these ranges and needn't reach their ends.
All inputs are finite; a program needn't handle non-finite values.
Results may differ from the reference program's by a relative error of at most 0.018.
Values may be sent and summed in bfloat16 or wider, within the bound.
No kernel may reach another device: no remote copies, remote signals or barrier semaphores. Data moves between devices by JAX's collectives and lax.ppermute only.
A program may use at most 192 MiB of HBM per device.

```python
import math
import jax
import jax.numpy as jnp
from jax import lax

D = 4096
HEADS = 16
NOPE = 128
ROPE = 64
VDIM = 128
KV_RANK = 512
FF = 6144
TOK_DEV = 256
TOKENS = 2048
N_TP = 4


def draw_pair(key):
    base = jax.random.fold_in(key, 7)
    key_one, key_two = jax.random.split(base, 2)
    width = NOPE + ROPE
    query = jax.random.truncated_normal(key_one, -6.0, 6.0, (TOKENS, HEADS, width), jnp.float32)
    rotary = jax.random.truncated_normal(key_two, -4.0, 4.0, (TOKENS, ROPE), jnp.float32)
    return (query.reshape(TOKENS, HEADS * width), rotary)


def draw_queries(key, part):
    return draw_pair(key)[0].astype(jnp.bfloat16)


def draw_rope_key(key, part):
    return draw_pair(key)[1].astype(jnp.bfloat16)


def draw_kv_weight(key, part):
    base = jax.random.fold_in(key, 11)
    shape = (KV_RANK, HEADS, NOPE + VDIM)
    matrix = jax.random.truncated_normal(base, -6.0, 6.0, shape, jnp.float32)
    ceiling = 3.0
    factor = ceiling ** (jnp.arange(HEADS, dtype=jnp.float32) / (HEADS - 1))
    scaled = jnp.concatenate([matrix[:, :, :NOPE], matrix[:, :, NOPE:] * factor[None, :, None]], axis=-1)
    return (scaled / math.sqrt(KV_RANK)).reshape(KV_RANK, HEADS * (NOPE + VDIM)).astype(jnp.bfloat16)


def shard_levels(rng, shape, pieces, low, top_value):
    level, own = 1.0, jax.random.fold_in(rng, 6)
    for dim, shards_of in pieces:
        heights = jnp.exp(jax.random.uniform(jax.random.fold_in(own, dim), (shards_of,), jnp.float32, low / len(pieces), top_value / len(pieces)))
        level = level * jnp.repeat(heights, shape[dim] // shards_of).reshape([-1 if axis == dim else 1 for axis in range(len(shape))])
    return level


def noise(own_key, dims, scale, reach, shards=(), kind=jnp.bfloat16):
    values = scale * jax.random.normal(own_key, dims, jnp.float32)
    if shards:
        values = values * shard_levels(own_key, dims, shards, -0.22, 0.18)
    return jnp.clip(values, -reach, reach).astype(kind)


def setup_inputs(seed: int = 0) -> dict:
    streams_of = jax.random.split(jax.random.key(seed), 13)
    return {
        "resid": noise(streams_of[0], (TOKENS, D), 1.0, 6.0, ((0, 8),)),
        "queries": draw_queries(jax.random.fold_in(streams_of[12], 71), 0),
        "latent": noise(streams_of[2], (TOKENS, KV_RANK), 1.0, 6.0, ((0, 8),)),
        "rope_key": draw_rope_key(jax.random.fold_in(streams_of[12], 71), 0),
        "lat_gain": jnp.clip(1.0 + 0.18 * jax.random.normal(streams_of[4], (KV_RANK,), jnp.float32), 0.1, 1.9),
        "kv_weight": draw_kv_weight(jax.random.fold_in(streams_of[12], 71), 0),
        "out_gain": jnp.clip(1.0 + 0.18 * jax.random.normal(streams_of[6], (HEADS * VDIM,), jnp.float32), 0.1, 1.9),
        "out_weight": noise(streams_of[7], (HEADS * VDIM, D), (HEADS * VDIM) ** -0.5, 0.125, ((0, 4),)),
        "ffn_gain": jnp.clip(1.0 + 0.18 * jax.random.normal(streams_of[8], (D,), jnp.float32), 0.1, 1.9),
        "gate_weight": noise(streams_of[9], (D, FF), D ** -0.5, 0.09375, ((0, 8), (1, 4))),
        "up_weight": noise(streams_of[10], (D, FF), D ** -0.5, 0.09375, ((0, 8), (1, 4))),
        "down_weight": noise(streams_of[11], (FF, D), FF ** -0.5, 0.078125, ((0, 4), (1, 8))),
    }


EPSILON = 1e-06
THETA = 10000.0

def rotate(values, places):
    half = values.shape[-1] // 2
    inverse = THETA ** (-jnp.arange(half, dtype=jnp.float32) / half)
    angle = places[..., None] * inverse
    cosine = jnp.cos(angle)
    sine = jnp.sin(angle)
    first = values[..., :half]
    second = values[..., half:]
    return jnp.concatenate([first * cosine - second * sine, first * sine + second * cosine], axis=-1)

def norm_rows(values, gain):
    wide = values.astype(jnp.float32)
    return wide * lax.rsqrt(lax.optimization_barrier(jnp.mean(wide * wide, axis=-1, keepdims=True)) + EPSILON) * gain.astype(jnp.float32)

def round_trip(values):
    return lax.optimization_barrier(values.astype(jnp.bfloat16)).astype(jnp.float32)

def reference(resid, queries, latent, rope_key, lat_gain, kv_weight, out_gain, out_weight, ffn_gain, gate_weight, up_weight, down_weight):
    total_rows = latent.shape[0]
    positions = jnp.arange(total_rows, dtype=jnp.int32)
    places = positions.astype(jnp.float32)
    normed = norm_rows(latent, lat_gain).astype(jnp.bfloat16)
    key_value = jnp.dot(normed, kv_weight, preferred_element_type=jnp.float32).astype(jnp.bfloat16)
    key_value = key_value.reshape(total_rows, HEADS, NOPE + VDIM).astype(jnp.float32)
    key_nope = key_value[:, :, :NOPE]
    values = key_value[:, :, NOPE:]
    key_rope = round_trip(rotate(rope_key.astype(jnp.float32), places))
    query = queries.reshape(total_rows, HEADS, NOPE + ROPE)
    query_nope = query[:, :, :NOPE].astype(jnp.float32)
    query_rope = round_trip(rotate(query[:, :, NOPE:].astype(jnp.float32), places[:, None]))
    scale = 1.0 / math.sqrt(NOPE + ROPE)
    blocks = total_rows // TOK_DEV

    def attend_block(index):
        first = (index * TOK_DEV).astype(jnp.int32)
        block_nope = lax.dynamic_slice_in_dim(query_nope, first, TOK_DEV, 0)
        block_rope = lax.dynamic_slice_in_dim(query_rope, first, TOK_DEV, 0)
        scores = jnp.einsum('qhd,khd->hqk', block_nope, key_nope) + jnp.einsum('qhr,kr->hqk', block_rope, key_rope)
        scores = scores * scale
        query_index = first + jnp.arange(TOK_DEV, dtype=jnp.int32)
        allowed = (positions[None, :] <= query_index[:, None])[None]
        scores = jnp.where(allowed, scores, -jnp.inf)
        highest = lax.optimization_barrier(jnp.max(scores, axis=-1, keepdims=True))
        weights = jnp.where(allowed, jnp.exp(scores - highest), 0.0)
        totals = lax.optimization_barrier(jnp.sum(weights, axis=-1))
        mixed = jnp.einsum('hqk,khd->qhd', round_trip(weights), values)
        return (mixed / jnp.transpose(totals)[:, :, None]).astype(jnp.bfloat16)
    attended = lax.map(attend_block, jnp.arange(blocks, dtype=jnp.int32))
    attended = attended.reshape(total_rows, HEADS * VDIM)
    normed_out = norm_rows(attended, out_gain).astype(jnp.bfloat16)
    group_width = HEADS * VDIM // N_TP
    attn_sum = jnp.zeros((total_rows, D), jnp.float32)
    for group in range(N_TP):
        lower = group * group_width
        part = jnp.dot(normed_out[:, lower:lower + group_width], out_weight[lower:lower + group_width], preferred_element_type=jnp.float32)
        attn_sum = attn_sum + round_trip(part)
    middle = (resid.astype(jnp.float32) + attn_sum).astype(jnp.bfloat16)
    normed_mid = norm_rows(middle, ffn_gain).astype(jnp.bfloat16)
    gate = jnp.dot(normed_mid, gate_weight, preferred_element_type=jnp.float32)
    upward = jnp.dot(normed_mid, up_weight, preferred_element_type=jnp.float32)
    hidden = (jax.nn.silu(gate) * upward).astype(jnp.bfloat16)
    group_units = FF // N_TP
    ffn_sum = jnp.zeros((total_rows, D), jnp.float32)
    for group in range(N_TP):
        lower = group * group_units
        part = jnp.dot(hidden[:, lower:lower + group_units], down_weight[lower:lower + group_units], preferred_element_type=jnp.float32)
        ffn_sum = ffn_sum + round_trip(part)
    return (middle.astype(jnp.float32) + ffn_sum).astype(jnp.bfloat16)
```

```python
import math

import jax
import jax.numpy as jnp
from jax import lax
from jax.sharding import PartitionSpec as P

HEADS = 16
NOPE = 128
ROPE = 64
VDIM = 128


EPSILON = 1e-06
THETA = 10000.0
LOWEST = -1e30


def rotate(values, places):
    half = values.shape[-1] // 2
    inverse = THETA ** (-jnp.arange(half, dtype=jnp.float32) / half)
    angle = places[..., None] * inverse
    cosine = jnp.cos(angle)
    sine = jnp.sin(angle)
    first = values[..., :half]
    second = values[..., half:]
    return jnp.concatenate(
        [first * cosine - second * sine, first * sine + second * cosine], axis=-1
    )


def norm_rows(values, gain):
    wide = values.astype(jnp.float32)
    return wide * lax.rsqrt(jnp.mean(wide * wide, axis=-1, keepdims=True) + EPSILON) * gain


def make_keys(latent_piece, rotary_piece, lat_gain, kv_weight):
    normed = norm_rows(latent_piece, lat_gain).astype(jnp.bfloat16)
    key_value = jnp.dot(normed, kv_weight, preferred_element_type=jnp.float32).astype(jnp.bfloat16)
    key_index = jnp.arange(latent_piece.shape[0], dtype=jnp.int32)
    key_rope = rotate(rotary_piece.astype(jnp.float32), key_index.astype(jnp.float32)).astype(
        jnp.bfloat16
    )
    return (key_value, key_rope)


def make_body(n_sp, n_tp):
    inner = 2 if n_sp % 2 == 0 else 1
    outer = n_sp // inner

    def shift(value, step):
        perm = [
            (o * inner + i, ((o + step) % outer) * inner + i)
            for o in range(outer)
            for i in range(inner)
        ]
        return lax.ppermute(value, "sp", perm)

    def with_partner(value, axis):
        if inner == 1:
            return value
        perm = [(o * inner + i, o * inner + 1 - i) for o in range(outer) for i in range(inner)]
        return jnp.concatenate([value, lax.ppermute(value, "sp", perm)], axis=axis)

    def own_first(value, place, axis):
        if inner == 1:
            return value
        return jnp.where(place == 0, value, jnp.flip(value, axis=axis))

    def body(
        resid,
        queries,
        latent,
        rope_key,
        lat_gain,
        kv_weight,
        out_gain,
        out_weight,
        ffn_gain,
        gate_weight,
        up_weight,
        down_weight,
    ):
        rows_here, width = resid.shape
        share = rows_here // n_tp
        sp_index = lax.axis_index("sp")
        tp_index = lax.axis_index("tp")
        first_row = sp_index * rows_here
        own_row = tp_index * share
        outer_index = sp_index // inner
        inner_index = sp_index % inner
        heads_here = queries.shape[1] // (NOPE + ROPE)
        rank = latent.shape[1]

        both = jnp.concatenate([latent, rope_key], axis=1)
        both = lax.all_gather(
            lax.dynamic_slice_in_dim(both, own_row, share, 0), ("sp", "tp"), axis=0, tiled=True
        )
        gate_up = jnp.concatenate(
            [with_partner(gate_weight, 0), with_partner(up_weight, 0)], axis=1
        )
        down = with_partner(down_weight, 1)

        query = queries.reshape(rows_here, heads_here, NOPE + ROPE)
        query_index = first_row + jnp.arange(rows_here, dtype=jnp.int32)
        query_nope = query[:, :, :NOPE]
        query_rope = rotate(
            query[:, :, NOPE:].astype(jnp.float32), query_index.astype(jnp.float32)[:, None]
        ).astype(jnp.bfloat16)
        scale = 1.0 / math.sqrt(NOPE + ROPE)
        key_value, key_rope = make_keys(both[:, :rank], both[:, rank:], lat_gain, kv_weight)
        length = key_value.shape[0]
        key_value = key_value.reshape(length, heads_here, NOPE + VDIM)
        key_index = jnp.arange(length, dtype=jnp.int32)
        scores = jnp.einsum(
            "qhd,khd->hqk", query_nope, key_value[:, :, :NOPE], preferred_element_type=jnp.float32
        )
        scores = (
            scores
            + jnp.einsum("qhr,kr->hqk", query_rope, key_rope, preferred_element_type=jnp.float32)
        ) * scale
        allowed = (key_index[None, :] <= query_index[:, None])[None]
        scores = jnp.where(allowed, scores, LOWEST)
        highest = jnp.max(scores, axis=-1)
        weights = jnp.where(allowed, jnp.exp(scores - highest[:, :, None]), 0.0)
        totals = jnp.sum(weights, axis=-1)
        weighted = jnp.einsum(
            "hqk,khd->qhd",
            weights.astype(jnp.bfloat16),
            key_value[:, :, NOPE:],
            preferred_element_type=jnp.float32,
        )
        attended = (weighted / jnp.transpose(totals)[:, :, None]).astype(jnp.bfloat16)
        attended_float = attended.reshape(rows_here, heads_here * VDIM).astype(jnp.float32)
        squares = lax.psum(jnp.sum(attended_float * attended_float, axis=1), "tp")
        normed_out = (
            attended_float * lax.rsqrt(squares / (HEADS * VDIM) + EPSILON)[:, None] * out_gain
        )
        normed_out = normed_out.astype(jnp.bfloat16)
        attn_sum = lax.psum_scatter(
            jnp.dot(normed_out, out_weight, preferred_element_type=jnp.float32).astype(
                jnp.bfloat16
            ),
            "tp",
            scatter_dimension=0,
            tiled=True,
        ).astype(jnp.float32)
        own_resid = lax.dynamic_slice_in_dim(resid, own_row, share, 0)
        middle = (own_resid.astype(jnp.float32) + attn_sum).astype(jnp.bfloat16)
        normed = norm_rows(middle, ffn_gain).astype(jnp.bfloat16)

        block = width // n_sp
        normed = own_first(normed.reshape(share, outer, inner, block), inner_index, 2)
        normed = normed.reshape(share, outer, inner * block)
        pieces = [
            shift(
                lax.dynamic_index_in_dim(normed, (outer_index + k) % outer, 1, keepdims=False), k
            )
            if k
            else lax.dynamic_index_in_dim(normed, outer_index, 1, keepdims=False)
            for k in range(outer)
        ]
        rows = lax.all_gather(jnp.stack(pieces), "tp", axis=1, tiled=True)
        units = gate_weight.shape[1]
        arrived = []
        for k in range(1, outer):
            part = jnp.dot(rows[k], gate_up, preferred_element_type=jnp.float32)
            arrived.append(shift(part.astype(jnp.bfloat16), -k))
        total = jnp.dot(rows[0], gate_up, preferred_element_type=jnp.float32)
        for part in arrived:
            total = total + part.astype(jnp.float32)
        hidden = (jax.nn.silu(total[:, :units]) * total[:, units:]).astype(jnp.bfloat16)
        terms = [
            jnp.dot(
                shift(hidden, k) if k else hidden, down, preferred_element_type=jnp.float32
            ).astype(jnp.bfloat16)
            for k in range(outer)
        ]
        summed = lax.psum_scatter(jnp.stack(terms), "tp", scatter_dimension=1, tiled=True)
        back = [shift(summed[k], -k) if k else summed[0] for k in range(outer)]
        turned = lax.dynamic_slice_in_dim(jnp.stack(back + back), outer - outer_index, outer, 0)
        ffn_sum = jnp.transpose(turned, (1, 0, 2)).reshape(share, outer, inner, block)
        ffn_sum = own_first(ffn_sum, inner_index, 2).reshape(share, width).astype(jnp.float32)
        return (middle.astype(jnp.float32) + ffn_sum).astype(jnp.bfloat16)

    return body


def solution(mesh):
    placed = (
        P("sp", None),
        P("sp", "tp"),
        P("sp", None),
        P("sp", None),
        P(),
        P(None, "tp"),
        P("tp"),
        P("tp", None),
        P(),
        P("sp", "tp"),
        P("sp", "tp"),
        P("tp", "sp"),
    )
    return jax.shard_map(
        make_body(mesh.shape["sp"], mesh.shape["tp"]),
        mesh=mesh,
        in_specs=placed,
        out_specs=P(("sp", "tp"), None),
        check_vma=False,
    )
```

```python
import math

import jax
import jax.numpy as jnp
from jax import lax
from jax.sharding import PartitionSpec as P

HEADS = 16
NOPE = 128
ROPE = 64
VDIM = 128


EPSILON = 1e-06
THETA = 10000.0
LOWEST = -1e30


def rotate(values, places):
    half = values.shape[-1] // 2
    inverse = THETA ** (-jnp.arange(half, dtype=jnp.float32) / half)
    angle = places[..., None] * inverse
    cosine = jnp.cos(angle)
    sine = jnp.sin(angle)
    first = values[..., :half]
    second = values[..., half:]
    return jnp.concatenate(
        [first * cosine - second * sine, first * sine + second * cosine], axis=-1
    )


def norm_rows(values, gain):
    wide = values.astype(jnp.float32)
    return wide * lax.rsqrt(jnp.mean(wide * wide, axis=-1, keepdims=True) + EPSILON) * gain


def make_keys(latent_piece, rotary_piece, key_index, lat_gain, kv_weight):
    normed = norm_rows(latent_piece, lat_gain).astype(jnp.bfloat16)
    key_value = jnp.dot(normed, kv_weight, preferred_element_type=jnp.float32).astype(jnp.bfloat16)
    key_rope = rotate(rotary_piece.astype(jnp.float32), key_index.astype(jnp.float32)).astype(
        jnp.bfloat16
    )
    return (key_value, key_rope)


def make_body(n_sp, n_tp):
    inner = 2 if n_sp % 2 == 0 else 1
    outer = n_sp // inner

    def shift(value, step):
        perm = [
            (o * inner + i, ((o + step) % outer) * inner + i)
            for o in range(outer)
            for i in range(inner)
        ]
        return lax.ppermute(value, "sp", perm)

    def with_partner(value, axis):
        if inner == 1:
            return value
        perm = [(o * inner + i, o * inner + 1 - i) for o in range(outer) for i in range(inner)]
        return jnp.concatenate([value, lax.ppermute(value, "sp", perm)], axis=axis)

    def own_first(value, place):
        if inner == 1:
            return value
        wide = value.shape[1] // n_sp
        swapped = [value[:, (b ^ 1) * wide : ((b ^ 1) + 1) * wide] for b in range(n_sp)]
        return jnp.where(place == 0, value, jnp.concatenate(swapped, axis=1))

    def across(value, step):
        return lax.ppermute(value, "tp", [(t, t ^ step) for t in range(n_tp)])

    def gather_tp(value):
        tail = value.shape
        step, axis = n_tp // 2, 0
        while step:
            value = jnp.stack([value, across(value, step)], axis=axis)
            step, axis = step // 2, axis + 1
        return value.reshape((n_tp,) + tail)

    def reduce_tp(value):
        tail = value.shape[1:]
        step = 1
        while step < n_tp:
            pair = value.astype(jnp.bfloat16).reshape((value.shape[0] // 2, 2) + tail)
            value = pair[:, 0].astype(jnp.float32) + across(pair[:, 1], step).astype(jnp.float32)
            step *= 2
        return value[0]

    def body(
        resid,
        queries,
        latent,
        rope_key,
        lat_gain,
        kv_weight,
        out_gain,
        out_weight,
        ffn_gain,
        gate_weight,
        up_weight,
        down_weight,
    ):
        rows_here, width = resid.shape
        share = rows_here // n_tp
        sp_index = lax.axis_index("sp")
        tp_index = lax.axis_index("tp")
        first_row = sp_index * rows_here
        own_row = tp_index * share
        outer_index = sp_index // inner
        inner_index = sp_index % inner
        heads_here = queries.shape[1] // (NOPE + ROPE)
        rank = latent.shape[1]

        both = jnp.concatenate([latent, rope_key], axis=1)
        both = lax.dynamic_slice_in_dim(both, own_row, share, 0)
        around = [
            lax.ppermute(both, "sp", [(s, (s + k) % n_sp) for s in range(n_sp)])
            for k in range(1, n_sp)
        ]
        both = gather_tp(jnp.stack([both] + around)).reshape(n_tp * n_sp * share, -1)
        owner = (sp_index - jnp.arange(n_sp, dtype=jnp.int32)) % n_sp
        slot = tp_index ^ jnp.arange(n_tp, dtype=jnp.int32)
        key_index = (
            owner[None, :, None] * rows_here
            + slot[:, None, None] * share
            + jnp.arange(share, dtype=jnp.int32)[None, None, :]
        ).reshape(-1)
        gate_both = with_partner(gate_weight, 0)
        up_both = with_partner(up_weight, 0)
        down = with_partner(down_weight, 1)
        gate_up = jnp.concatenate([gate_both, up_both], axis=1)

        query = queries.reshape(rows_here, heads_here, NOPE + ROPE)
        query_index = first_row + jnp.arange(rows_here, dtype=jnp.int32)
        query_nope = query[:, :, :NOPE]
        query_rope = rotate(
            query[:, :, NOPE:].astype(jnp.float32), query_index.astype(jnp.float32)[:, None]
        ).astype(jnp.bfloat16)
        scale = 1.0 / math.sqrt(NOPE + ROPE)
        key_value, key_rope = make_keys(both[:, :rank], both[:, rank:], key_index, lat_gain, kv_weight)
        length = key_value.shape[0]
        key_value = key_value.reshape(length, heads_here, NOPE + VDIM)
        scores = jnp.einsum(
            "qhd,khd->hqk", query_nope, key_value[:, :, :NOPE], preferred_element_type=jnp.float32
        )
        scores = (
            scores
            + jnp.einsum("qhr,kr->hqk", query_rope, key_rope, preferred_element_type=jnp.float32)
        ) * scale
        allowed = (key_index[None, :] <= query_index[:, None])[None]
        scores = jnp.where(allowed, scores, LOWEST)
        highest = jnp.max(scores, axis=-1)
        weights = jnp.where(allowed, jnp.exp(scores - highest[:, :, None]), 0.0)
        totals = jnp.sum(weights, axis=-1)
        weighted = jnp.einsum(
            "hqk,khd->qhd",
            weights.astype(jnp.bfloat16),
            key_value[:, :, NOPE:],
            preferred_element_type=jnp.float32,
        )
        attended = (weighted / jnp.transpose(totals)[:, :, None]).astype(jnp.bfloat16)
        attended_float = attended.reshape(rows_here, heads_here * VDIM).astype(jnp.float32)
        squares = lax.psum(jnp.sum(attended_float * attended_float, axis=1), "tp")
        normed_out = (
            attended_float * lax.rsqrt(squares / (HEADS * VDIM) + EPSILON)[:, None] * out_gain
        )
        normed_out = normed_out.astype(jnp.bfloat16).reshape(n_tp, share, heads_here * VDIM)
        normed_out = jnp.concatenate(
            [
                lax.dynamic_index_in_dim(normed_out, tp_index ^ j, 0, keepdims=False)
                for j in range(n_tp)
            ]
        )
        product = jnp.dot(normed_out, out_weight, preferred_element_type=jnp.float32)
        attn_sum = reduce_tp(product.astype(jnp.bfloat16).reshape(n_tp, share, width))
        own_resid = lax.dynamic_slice_in_dim(resid, own_row, share, 0)
        middle = (own_resid.astype(jnp.float32) + attn_sum).astype(jnp.bfloat16)
        normed = norm_rows(middle, ffn_gain).astype(jnp.bfloat16)

        block = width // n_sp
        normed = own_first(normed, inner_index)
        span = inner * block
        pieces = [
            lax.dynamic_slice_in_dim(normed, (outer_index + k) % outer * span, span, 1)
            for k in range(outer)
        ]
        pieces = [shift(piece, k) if k else piece for k, piece in enumerate(pieces)]
        rows = gather_tp(jnp.stack(pieces))
        rows = [rows[:, k].reshape(rows_here, span) for k in range(outer)]
        units = gate_weight.shape[1]
        arrived = []
        for k in range(1, outer):
            part = jnp.dot(rows[k], gate_up, preferred_element_type=jnp.float32)
            arrived.append(shift(part.astype(jnp.bfloat16), -k))
        total = lax.optimization_barrier(
            jnp.dot(rows[0], gate_up, preferred_element_type=jnp.float32)
        )
        for part in arrived:
            total = total + part.astype(jnp.float32)
        hidden = (jax.nn.silu(total[:, :units]) * total[:, units:]).astype(jnp.bfloat16)
        terms = [
            jnp.dot(
                shift(hidden, k) if k else hidden, down, preferred_element_type=jnp.float32
            ).astype(jnp.bfloat16)
            for k in range(outer)
        ]
        terms = [term.reshape(n_tp, share, span) for term in terms]
        summed = reduce_tp(jnp.stack(terms, axis=1)).astype(jnp.bfloat16)
        back = [shift(summed[k], -k) if k else summed[0] for k in range(outer)]
        back = jnp.concatenate(back + back, axis=1)
        ffn_sum = lax.dynamic_slice_in_dim(back, (outer - outer_index) * span, width, 1)
        ffn_sum = own_first(ffn_sum, inner_index).astype(jnp.float32)
        return (middle.astype(jnp.float32) + ffn_sum).astype(jnp.bfloat16)

    return body


def solution(mesh):
    placed = (
        P("sp", None),
        P("sp", "tp"),
        P("sp", None),
        P("sp", None),
        P(),
        P(None, "tp"),
        P("tp"),
        P("tp", None),
        P(),
        P("sp", "tp"),
        P("sp", "tp"),
        P("tp", "sp"),
    )
    body = make_body(mesh.shape["sp"], mesh.shape["tp"])

    return jax.shard_map(
        body,
        mesh=mesh,
        in_specs=placed,
        out_specs=P(("sp", "tp"), None),
        check_vma=False,
    )
```
